128 devices in a mesh: ep: 128 (over z, y, x, core).
Axes of the slice: x: 4, y: 4, z: 4, core: 2. Of those that a mesh axis runs over, the one named last changes fastest.
Arguments:
- tokens: bfloat16 [4096, 3072], P('ep'), may hold values from -6 to 6
- norm_gain: float32 [3072], replicated, may hold values from 0.1 to 1.9
- expert_ids: int32 [4096, 4], P('ep'), may hold values from 0 to 127, as said below
- expert_scores: float32 [4096, 4], P('ep'), may hold values from -100 to 180
- group_prob: float32 [4096], P('ep'), may hold values from 0.25 to 1
- gate_weight: bfloat16 [128, 3072, 384], P('ep'), may hold values from -0.109375 to 0.109375
- up_weight: bfloat16 [128, 3072, 384], P('ep'), may hold values from -0.109375 to 0.109375
- down_weight: bfloat16 [128, 384, 3072], P('ep'), may hold values from -0.3125 to 0.3125
Outputs:
- combined: bfloat16 [4096, 3072], P('ep')
The draws below stay inside these ranges and needn't reach their ends.
Inputs may be any that keep to these rules, and one draw needn't show every extreme that they name: `expert_ids`: the 4 ids of a row are different and lie in one group of 32 consecutive experts. Among the rows of one device no expert is named by more than 4 rows, and in every draw some expert is named by exactly 4 rows of one device.
All inputs are finite; a program needn't handle non-finite values.
Results may differ from the reference program's by a relative error of at most 0.0085.
Values may be sent and summed in bfloat16 or wider, within the bound.
A program may use at most 128 MiB of HBM per device.

```python
import jax
import jax.numpy as jnp
from jax import lax

D = 3072
FFE = 384
GROUPS = 4
TOP_K = 4
TOK_DEV = 32
EXPERTS = 128
TOKENS = 4096
MOST = 4
N_EP = 128


def draw_expert_ids(key, part):
    blocks_count = TOKENS // TOK_DEV
    group_size = EXPERTS // GROUPS
    hot_count = (MOST - 1) * group_size // TOP_K + 1
    keys = jax.random.split(jax.random.fold_in(key, 11), 5)
    group_order = jax.random.permutation(keys[0], GROUPS)
    chosen_rank = jnp.min(jax.random.randint(keys[1], (3, blocks_count, TOK_DEV), 0, GROUPS), axis=0)
    hot_rank = jnp.min(jax.random.randint(keys[2], (3, blocks_count, 1), 0, GROUPS), axis=0)
    position = jnp.arange(TOK_DEV)[None, :]
    group_index = group_order[jnp.where(position < hot_count, hot_rank, chosen_rank)]
    earlier_mask = (group_index[:, :, None] == group_index[:, None, :]) & (jnp.arange(TOK_DEV)[None, None, :] < jnp.arange(TOK_DEV)[None, :, None])
    earlier = jnp.sum(earlier_mask.astype(jnp.int32), axis=2)
    starts = jax.random.randint(keys[3], (blocks_count, GROUPS), 0, group_size)
    start_here = jnp.take_along_axis(starts, group_index, axis=1)
    local_ids = (start_here[:, :, None] + earlier[:, :, None] * TOP_K + jnp.arange(TOP_K)[None, None, :]) % group_size
    global_ids = group_index[:, :, None] * group_size + local_ids
    return global_ids.reshape(TOKENS, TOP_K).astype(jnp.int32)


def draw_expert_scores(key, part):
    keys = jax.random.split(jax.random.fold_in(key, 23), 3)
    base_scores = jnp.clip(jax.random.normal(keys[0], (TOKENS, TOP_K), jnp.float32), -6.0, 6.0) * 1.5
    return base_scores.astype(jnp.float32)


def levels(rng, dims, shards, low, high):
    def one(axis_at, parts):
        heights = jax.random.uniform(jax.random.fold_in(jax.random.fold_in(rng, 6), axis_at), (parts,), jnp.float32, low / len(shards), high / len(shards))
        return jnp.repeat(jnp.exp(heights), dims[axis_at] // parts).reshape((-1,) + (1,) * (len(dims) - axis_at - 1))

    level = one(*shards[0])
    for cut in shards[1:]:
        level = level * one(*cut)
    return level


def gaussian(key, dims, deviation, reach, shards=(), kind=jnp.bfloat16):
    drawn = deviation * jax.random.normal(key, dims, jnp.float32)
    if shards:
        drawn = drawn * levels(key, dims, shards, -0.22, 0.18)
    return jnp.clip(drawn, -reach, reach).astype(kind)


def setup_inputs(seed: int = 0) -> dict:
    streams_of = jax.random.split(jax.random.key(seed), 9)
    return {
        "tokens": gaussian(streams_of[0], (TOKENS, D), 1.0, 6.0, ((0, 128),)),
        "norm_gain": jnp.clip(1.0 + 0.18 * jax.random.normal(streams_of[1], (D,), jnp.float32), 0.1, 1.9),
        "expert_ids": draw_expert_ids(jax.random.fold_in(streams_of[8], 71), 0),
        "expert_scores": draw_expert_scores(jax.random.fold_in(streams_of[8], 71), 0),
        "group_prob": jnp.clip(0.25 + 0.75 * jax.random.uniform(streams_of[4], (TOKENS,), jnp.float32) ** levels(streams_of[4], (TOKENS,), ((0, 128),), -0.2, 0.2), 0.25, 1.0),
        "gate_weight": gaussian(streams_of[5], (EXPERTS, D, FFE), D ** -0.5, 0.109375, ((0, 128),)),
        "up_weight": gaussian(streams_of[6], (EXPERTS, D, FFE), D ** -0.5, 0.109375, ((0, 128),)),
        "down_weight": gaussian(streams_of[7], (EXPERTS, FFE, D), FFE ** -0.5, 0.3125, ((0, 128),)),
    }


eps_norm = 1e-05

def layer_norm(tokens, norm_gain):
    values = tokens.astype(jnp.float32)
    average = lax.optimization_barrier(jnp.mean(values, axis=1, keepdims=True))
    centred = values - average
    variance = lax.optimization_barrier(jnp.mean(centred * centred, axis=1, keepdims=True))
    return (centred * lax.rsqrt(variance + eps_norm) * norm_gain[None, :]).astype(jnp.bfloat16)

def mixing_weights(expert_scores, group_prob):
    shifted = expert_scores - lax.optimization_barrier(jnp.max(expert_scores, axis=1, keepdims=True))
    exp_scores = jnp.exp(shifted)
    return exp_scores / lax.optimization_barrier(jnp.sum(exp_scores, axis=1, keepdims=True)) * group_prob[:, None]

def expert_rows(flat_rows, gate_matrix, up_matrix, down_matrix):
    gate_act = jnp.dot(flat_rows, gate_matrix, preferred_element_type=jnp.float32)
    up_act = jnp.dot(flat_rows, up_matrix, preferred_element_type=jnp.float32)
    hidden = (jax.nn.silu(gate_act) * up_act).astype(jnp.bfloat16)
    return jnp.dot(hidden, down_matrix, preferred_element_type=jnp.float32).astype(jnp.bfloat16)

def reference(tokens, norm_gain, expert_ids, expert_scores, group_prob, gate_weight, up_weight, down_weight):
    normed = layer_norm(tokens, norm_gain)
    weights_tok = mixing_weights(expert_scores, group_prob)
    capacity = N_EP * MOST
    slot_iota = jnp.arange(capacity, dtype=jnp.int32)

    def per_expert(running, expert_index):
        matches = expert_ids == expert_index
        chosen = jnp.any(matches, axis=1)
        own_weight = lax.optimization_barrier(jnp.sum(jnp.where(matches, weights_tok, 0.0), axis=1))
        slot_token = jnp.nonzero(chosen, size=capacity, fill_value=0)[0].astype(jnp.int32)
        filled = slot_iota < jnp.sum(chosen.astype(jnp.int32))
        results = expert_rows(normed[slot_token], gate_weight[expert_index], up_weight[expert_index], down_weight[expert_index])
        slot_scale = jnp.where(filled, own_weight[slot_token], 0.0)
        running = running.at[slot_token].add(slot_scale[:, None] * results.astype(jnp.float32))
        return (running, None)
    start = jnp.zeros((TOKENS, D), jnp.float32)
    mixture, _ = lax.scan(per_expert, start, jnp.arange(EXPERTS, dtype=jnp.int32))
    return mixture.astype(jnp.bfloat16)
```

```python
import jax
import jax.numpy as jnp
from jax import lax
from jax.experimental import pallas as pl
from jax.experimental.pallas import tpu as pltpu
from jax.sharding import PartitionSpec as P

eps_norm = 1e-05
MESH = pl.DeviceIdType.MESH

LINE = 4
SLOTS = 4
TOK = 32
CHUNK = 1024
CHUNKS = 3
ROWS = 256
FFE = 384
STRIDE = (7, 11, 13)


def iota(shape, dim):
    return lax.broadcasted_iota(jnp.int32, shape, dim)


def device(z, y, x, c):
    return ((z * 4 + y) * 4 + x) * 2 + c


def step_kernel(
    tok_ref, gain_ref, ids_ref, score_ref, prob_ref, gate_hbm, up_hbm, down_hbm,
    out_ref,
    w_in, w_out, xa, aux, sb, rb, xp, ob, gb, tsum, tb, fb, wm_hi, wm_lo,
    w_sem, s1, r1, sa, ra, s2, r2, s3, r3, s4, r4,
):
    me = lax.axis_index("ep")
    z, y, x, c = me // 32, (me // 8) % 4, (me // 2) % 4, me % 2
    other = 1 - c
    pos = (x, y, z)
    plane = ((z, y), (z, x), (x, y))

    def line_peer(q, p, core):
        return (
            device(z, y, p, core),
            device(z, p, x, core),
            device(p, y, x, core),
        )[q]

    def plane_peer(q, a, b, core):
        return (
            device(a, b, x, core),
            device(a, y, b, core),
            device(z, b, a, core),
        )[q]

    def rel(value, step):
        return (value + step) % 4

    weights = [
        pltpu.make_async_copy(gate_hbm.at[0], w_in.at[:, pl.ds(0, FFE)], w_sem.at[0]),
        pltpu.make_async_copy(up_hbm.at[0], w_in.at[:, pl.ds(FFE, FFE)], w_sem.at[1]),
        pltpu.make_async_copy(down_hbm.at[0], w_out, w_sem.at[2]),
    ]
    for copy in weights:
        copy.start()

    barrier = pltpu.get_barrier_semaphore()
    for q in range(CHUNKS):
        for step in range(1, LINE):
            for core in (c, other):
                pl.semaphore_signal(
                    barrier, inc=1, device_id=(line_peer(q, rel(pos[q], step), core),),
                    device_id_type=MESH,
                )
    pl.semaphore_signal(barrier, inc=1, device_id=(device(z, y, x, other),), device_id_type=MESH)

    values = tok_ref[...].astype(jnp.float32)
    centred = values - jnp.mean(values, axis=1, keepdims=True)
    variance = jnp.mean(centred * centred, axis=1, keepdims=True)
    normed = (centred * lax.rsqrt(variance + eps_norm) * gain_ref[...]).astype(jnp.bfloat16)
    for q in range(CHUNKS):
        xa[q, pl.ds(pos[q], 1)] = normed[:, q * CHUNK:(q + 1) * CHUNK][None]

    ids = ids_ref[...]
    scores = score_ref[...]
    exp_scores = jnp.exp(scores - jnp.max(scores, axis=1, keepdims=True))
    prob = jnp.sum(
        jnp.where(iota((TOK, TOK), 0) == iota((TOK, TOK), 1), prob_ref[...], 0.0),
        axis=1, keepdims=True,
    )
    mixing = exp_scores / jnp.sum(exp_scores, axis=1, keepdims=True) * prob
    lane = iota((TOK, 128), 1)
    matches = [ids[:, k:k + 1] == lane for k in range(4)]
    named = sum(jnp.where(match, 1.0, 0.0) for match in matches)
    earlier = jnp.where(iota((TOK, TOK), 1) < iota((TOK, TOK), 0), 1.0, 0.0)
    rank = jnp.dot(
        earlier.astype(jnp.bfloat16), named.astype(jnp.bfloat16),
        preferred_element_type=jnp.float32,
    )
    table = jnp.zeros((TOK, 128), jnp.float32)
    for k in range(4):
        slot = jnp.sum(jnp.where(matches[k], rank, 0.0), axis=1, keepdims=True)
        code = ids[:, k:k + 1].astype(jnp.float32) * 16.0 + slot
        table = jnp.where(lane == k, code, table)
        table = jnp.where(lane == 4 + k, mixing[:, k:k + 1], table)
    own_aux = jnp.transpose(jnp.concatenate([table] * 4, axis=0))[0:8]
    for q in range(CHUNKS):
        aux[q, pl.ds(pos[q], 1)] = own_aux[None]

    pl.semaphore_wait(barrier, 19)

    for step in (1, 3, 2):
        for q in range(CHUNKS):
            peer = (line_peer(q, rel(pos[q], step), c),)
            pltpu.make_async_remote_copy(
                src_ref=aux.at[q, pos[q]], dst_ref=aux.at[q, pos[q]],
                send_sem=sa.at[q], recv_sem=ra.at[q], device_id=peer, device_id_type=MESH,
            ).start()
            pltpu.make_async_remote_copy(
                src_ref=xa.at[q, pos[q]], dst_ref=xa.at[q, pos[q]],
                send_sem=s1.at[q], recv_sem=r1.at[q], device_id=peer, device_id_type=MESH,
            ).start()

    def bulk(ref, q, count, send_sem, recv_sem):
        part = ref.at[q, pl.ds(0, count)]
        return pltpu.make_async_remote_copy(
            src_ref=part, dst_ref=part, send_sem=send_sem, recv_sem=recv_sem,
            device_id=(me,), device_id_type=MESH,
        )

    def row_code(q, h, shape, dim):
        r = iota(shape, dim)
        a, b, low = r >> 6, (r >> 4) & 3, r & 15
        core = c if h == 0 else other
        return (plane_peer(q, a, b, core) * 16 + low).astype(jnp.float32)

    def line_aux(q):
        group = iota((8, 128), 1) >> 5
        found = jnp.zeros((8, 128), jnp.float32)
        for s in range(LINE):
            found = jnp.where(group == s, aux[q, s], found)
        return found + jnp.where(iota((8, 128), 0) < 4, (group * 4).astype(jnp.float32), 0.0)

    for q in range(CHUNKS):
        bulk(aux, q, LINE - 1, sa.at[q], ra.at[q]).wait_recv()
    found = [line_aux(q) for q in range(CHUNKS)]

    def pick(q, h):
        want = row_code(q, h, (ROWS, 128), 0)
        hit = found[q][0:1] == want
        for k in range(1, 4):
            hit = hit | (found[q][k:k + 1] == want)
        return jnp.where(hit, 1.0, 0.0).astype(jnp.bfloat16)

    def select(q, h):
        rows = jnp.dot(
            pick(q, h), xa[q].reshape(LINE * TOK, CHUNK), preferred_element_type=jnp.float32
        )
        sb[q, h * 16:(h + 1) * 16] = rows.astype(jnp.bfloat16).reshape(16, 16, CHUNK)

    def exchange(src, dst, h, send_sem, recv_sem):
        core = c if h == 0 else other

        def body(t, carry):
            for q in range(CHUNKS):
                turn = (t * STRIDE[q]) % 16
                a, b = rel(plane[q][0], turn // 4), rel(plane[q][1], turn % 4)
                pltpu.make_async_remote_copy(
                    src_ref=src.at[q, h * 16 + a * 4 + b],
                    dst_ref=dst.at[q, h * 16 + plane[q][0] * 4 + plane[q][1]],
                    send_sem=send_sem.at[h * 3 + q], recv_sem=recv_sem.at[h * 3 + q],
                    device_id=(plane_peer(q, a, b, core),), device_id_type=MESH,
                ).start()
            return carry

        lax.fori_loop(1 - h, 16, body, 0)
        if h == 0:
            for q in range(CHUNKS):
                mine = plane[q][0] * 4 + plane[q][1]
                dst[q, pl.ds(mine, 1)] = src[q, pl.ds(mine, 1)]

    for q in range(CHUNKS):
        bulk(xa, q, LINE - 1, s1.at[q], r1.at[q]).wait_recv()
        select(q, 0)
    exchange(sb, rb, 0, s2, r2)
    for q in range(CHUNKS):
        select(q, 1)
    exchange(sb, rb, 1, s2, r2)

    for q in range(CHUNKS):
        cols = jnp.transpose(
            jnp.concatenate([found[q], jnp.zeros((120, 128), jnp.float32)], axis=0)
        )
        for h in range(2):
            want = row_code(q, h, (128, ROWS), 1)
            scale = jnp.zeros((128, ROWS), jnp.float32)
            for k in range(4):
                scale = jnp.where(cols[:, k:k + 1] == want, cols[:, 4 + k:5 + k], scale)
            high = scale.astype(jnp.bfloat16)
            wm_hi[q, h] = high
            wm_lo[q, h] = (scale - high.astype(jnp.float32)).astype(jnp.bfloat16)

    def swap(high, low):
        i, j = iota((ROWS, ROWS), 0), iota((ROWS, ROWS), 1)
        rest = 255 - (3 << high) - (3 << low)
        moved = (i & rest) | (((i >> high) & 3) << low) | (((i >> low) & 3) << high)
        return jnp.where(moved == j, 1.0, 0.0).astype(jnp.bfloat16)

    orders = (None, swap(4, 2), swap(6, 2))

    def in_order(q, rows):
        if q == 0:
            return rows
        return jnp.dot(orders[q], rows, preferred_element_type=jnp.float32).astype(jnp.bfloat16)

    for copy in weights:
        copy.wait()
    for h in range(2):
        for q in range(CHUNKS):
            bulk(rb, q, 15 + h, s2.at[h * 3 + q], r2.at[h * 3 + q]).wait_recv()
            rows = rb[q, h * 16:(h + 1) * 16].reshape(ROWS, CHUNK)
            xp[:, q * CHUNK:(q + 1) * CHUNK] = in_order(q, rows)
        acts = jnp.dot(xp[...], w_in[...], preferred_element_type=jnp.float32)
        gate_act, up_act = acts[:, :FFE], acts[:, FFE:]
        hidden = (gate_act * jax.nn.sigmoid(gate_act) * up_act).astype(jnp.bfloat16)
        for q in range(CHUNKS):
            made = jnp.dot(
                in_order(q, hidden), w_out[:, q * CHUNK:(q + 1) * CHUNK],
                preferred_element_type=jnp.float32,
            )
            ob[q, h * 16:(h + 1) * 16] = made.astype(jnp.bfloat16).reshape(16, 16, CHUNK)
        exchange(ob, gb, h, s3, r3)

    for h in range(2):
        for q in range(CHUNKS):
            bulk(gb, q, 15 + h, s3.at[h * 3 + q], r3.at[h * 3 + q]).wait_recv()
            rows = gb[q, h * 16:(h + 1) * 16].reshape(ROWS, CHUNK)
            part = jnp.dot(wm_hi[q, h], rows, preferred_element_type=jnp.float32)
            part += jnp.dot(wm_lo[q, h], rows, preferred_element_type=jnp.float32)
            if h == 0:
                tsum[q] = part.reshape(LINE, TOK, CHUNK)
            else:
                part = tsum[q] + part.reshape(LINE, TOK, CHUNK)
                tsum[q] = part
                tb[q] = part.astype(jnp.bfloat16)
                for step in (2, 1, 3):
                    there = rel(pos[q], step)
                    pltpu.make_async_remote_copy(
                        src_ref=tb.at[q, there], dst_ref=fb.at[q, pos[q]],
                        send_sem=s4.at[q], recv_sem=r4.at[q],
                        device_id=(line_peer(q, there, c),), device_id_type=MESH,
                    ).start()

    for q in range(CHUNKS):
        bulk(fb, q, LINE - 1, s4.at[q], r4.at[q]).wait_recv()
        total = tsum[q, pl.ds(pos[q], 1)][0]
        for step in range(1, LINE):
            total += fb[q, pl.ds(rel(pos[q], step), 1)][0].astype(jnp.float32)
        out_ref[:, q * CHUNK:(q + 1) * CHUNK] = total.astype(jnp.bfloat16)

    for q in range(CHUNKS):
        bulk(aux, q, LINE - 1, sa.at[q], ra.at[q]).wait_send()
        bulk(xa, q, LINE - 1, s1.at[q], r1.at[q]).wait_send()
        bulk(tb, q, LINE - 1, s4.at[q], r4.at[q]).wait_send()
        for h in range(2):
            bulk(sb, q, 15 + h, s2.at[h * 3 + q], r2.at[h * 3 + q]).wait_send()
            bulk(ob, q, 15 + h, s3.at[h * 3 + q], r3.at[h * 3 + q]).wait_send()


def local(
    tokens, norm_gain, expert_ids, expert_scores, group_prob, gate_weight, up_weight, down_weight
):
    vmem = pl.BlockSpec(memory_space=pltpu.VMEM)
    hbm = pl.BlockSpec(memory_space=pl.ANY)
    bf16, f32 = jnp.bfloat16, jnp.float32
    dma = pltpu.SemaphoreType.DMA
    rows = pltpu.VMEM((CHUNKS, 32, 16, CHUNK), bf16)
    line = (CHUNKS, LINE, TOK, CHUNK)
    return pl.pallas_call(
        step_kernel,
        out_shape=jax.ShapeDtypeStruct(tokens.shape, bf16),
        in_specs=[vmem] * 5 + [hbm] * 3,
        out_specs=vmem,
        scratch_shapes=[
            pltpu.VMEM((CHUNKS * CHUNK, 2 * FFE), bf16),
            pltpu.VMEM((FFE, CHUNKS * CHUNK), bf16),
            pltpu.VMEM(line, bf16),
            pltpu.VMEM((CHUNKS, LINE, 8, 128), f32),
            rows,
            rows,
            pltpu.VMEM((ROWS, CHUNKS * CHUNK), bf16),
            rows,
            rows,
            pltpu.VMEM(line, f32),
            pltpu.VMEM(line, bf16),
            pltpu.VMEM(line, bf16),
            pltpu.VMEM((CHUNKS, 2, 128, ROWS), bf16),
            pltpu.VMEM((CHUNKS, 2, 128, ROWS), bf16),
            dma((3,)),
            dma((3,)), dma((3,)),
            dma((3,)), dma((3,)),
            dma((6,)), dma((6,)),
            dma((6,)), dma((6,)),
            dma((3,)), dma((3,)),
        ],
        compiler_params=pltpu.CompilerParams(
            collective_id=0, has_side_effects=True, vmem_limit_bytes=60 * 2**20
        ),
        name="expert_step",
    )(
        tokens, norm_gain[None, :], expert_ids, expert_scores, group_prob[None, :],
        gate_weight, up_weight, down_weight,
    )


def solution(mesh):
    in_specs = (
        P("ep", None),
        P(),
        P("ep", None),
        P("ep", None),
        P("ep"),
        P("ep", None, None),
        P("ep", None, None),
        P("ep", None, None),
    )
    out_specs = P("ep", None)
    return jax.shard_map(local, mesh=mesh, in_specs=in_specs, out_specs=out_specs, check_vma=False)
```

```python
import jax
import jax.numpy as jnp
from jax import lax
from jax.experimental import pallas as pl
from jax.experimental.pallas import tpu as pltpu
from jax.sharding import PartitionSpec as P

eps_norm = 1e-05
MESH = pl.DeviceIdType.MESH

LINE = 4
SLOTS = 4
TOK = 32
KINDS = 3
CHUNK = 512
CHUNKS = 6
PARTS = ((0, 1, 2), (3, 4, 5))
ROWS = 256
FFE = 384
STRIDE = (7, 11, 13)


def iota(shape, dim):
    return lax.broadcasted_iota(jnp.int32, shape, dim)


def device(z, y, x, c):
    return ((z * 4 + y) * 4 + x) * 2 + c


def columns(j):
    return slice(j * CHUNK, (j + 1) * CHUNK)


def step_kernel(
    tok_hbm, gain_hbm, ids_hbm, score_hbm, prob_hbm, gate_hbm, up_hbm, down_hbm,
    parts_ref,
    tok_ref, gain_ref, ids_ref, score_ref, prob_ref, spread,
    w_in, w_out, xa, aux, picks, sb, rb, xp, ob, gb, tsum, tb, wm_hi, wm_lo,
    in_sem, w_sem, own_sem, s1, r1, sa, ra, s2, r2, s3, r3, s4, r4,
):
    me = lax.axis_index("ep")
    z, y, x, c = me // 32, (me // 8) % 4, (me // 2) % 4, me % 2
    other = 1 - c
    pos = (x, y, z)
    plane = ((z, y), (z, x), (x, y))

    def line_peer(q, p, core):
        return (
            device(z, y, p, core),
            device(z, p, x, core),
            device(p, y, x, core),
        )[q]

    def plane_peer(q, a, b, core):
        return (
            device(a, b, x, core),
            device(a, y, b, core),
            device(z, b, a, core),
        )[q]

    def rel(value, step):
        return (value + step) % 4

    barrier = pltpu.get_barrier_semaphore()
    for q in range(KINDS):
        for step in range(1, LINE):
            for core in (c, other):
                pl.semaphore_signal(
                    barrier, inc=1, device_id=(line_peer(q, rel(pos[q], step), core),),
                    device_id_type=MESH,
                )
    pl.semaphore_signal(barrier, inc=1, device_id=(device(z, y, x, other),), device_id_type=MESH)

    smalls = [
        pltpu.make_async_copy(src, dst, in_sem.at[i])
        for i, (src, dst) in enumerate((
            (tok_hbm, tok_ref), (gain_hbm, gain_ref), (ids_hbm, ids_ref),
            (score_hbm, score_ref), (prob_hbm, prob_ref),
        ))
    ]
    for copy in smalls:
        copy.start()
    weights = [
        pltpu.make_async_copy(gate_hbm.at[0], w_in.at[:, pl.ds(0, FFE)], w_sem.at[0]),
        pltpu.make_async_copy(up_hbm.at[0], w_in.at[:, pl.ds(FFE, FFE)], w_sem.at[1]),
        pltpu.make_async_copy(down_hbm.at[0], w_out, w_sem.at[2]),
    ]
    for copy in weights:
        copy.start()
    for copy in smalls:
        copy.wait()

    ids = ids_ref[...]
    scores = score_ref[...]
    exp_scores = jnp.exp(scores - jnp.max(scores, axis=0, keepdims=True))
    mixing = exp_scores / jnp.sum(exp_scores, axis=0, keepdims=True) * prob_ref[...]
    expert = iota((128, TOK), 0)
    matches = [ids[k:k + 1] == expert for k in range(4)]
    named = sum(jnp.where(match, 1.0, 0.0) for match in matches)
    earlier = jnp.where(iota((TOK, TOK), 0) < iota((TOK, TOK), 1), 1.0, 0.0)
    rank = jnp.dot(
        named.astype(jnp.bfloat16), earlier.astype(jnp.bfloat16),
        preferred_element_type=jnp.float32,
    )
    spread[...] = jnp.zeros((8, 128), jnp.float32)
    for k in range(4):
        slot = jnp.sum(jnp.where(matches[k], rank, 0.0), axis=0, keepdims=True)
        spread[k:k + 1, 0:TOK] = ids[k:k + 1].astype(jnp.float32) * 16.0 + slot
        spread[4 + k:5 + k, 0:TOK] = mixing[k:k + 1]
    own_aux = spread[...]
    own_aux = own_aux + pltpu.roll(own_aux, TOK, 1)
    own_aux = own_aux + pltpu.roll(own_aux, 2 * TOK, 1)
    for q in range(KINDS):
        aux[q, pl.ds(pos[q], 1)] = own_aux[None]

    values = tok_ref[...].astype(jnp.float32)
    average = jnp.mean(values, axis=1, keepdims=True)
    centred = values - average
    scale = lax.rsqrt(jnp.mean(centred * centred, axis=1, keepdims=True) + eps_norm)

    def normalise(part):
        for j in part:
            values = tok_ref[:, columns(j)].astype(jnp.float32)
            normed = (values - average) * scale * gain_ref[:, columns(j)]
            xa[j, pl.ds(pos[j % 3], 1)] = normed.astype(jnp.bfloat16)[None]

    def gather(part):
        for step in (2, 1, 3):
            for j in part:
                q = j % 3
                pltpu.make_async_remote_copy(
                    src_ref=xa.at[j, pos[q]], dst_ref=xa.at[j, pos[q]],
                    send_sem=s1.at[j], recv_sem=r1.at[j],
                    device_id=(line_peer(q, rel(pos[q], step), c),), device_id_type=MESH,
                ).start()

    normalise(PARTS[0])
    pl.semaphore_wait(barrier, 19)
    for step in (2, 1, 3):
        for q in range(KINDS):
            pltpu.make_async_remote_copy(
                src_ref=aux.at[q, pos[q]], dst_ref=aux.at[q, pos[q]],
                send_sem=sa.at[q], recv_sem=ra.at[q],
                device_id=(line_peer(q, rel(pos[q], step), c),), device_id_type=MESH,
            ).start()
    gather(PARTS[0])
    normalise(PARTS[1])
    gather(PARTS[1])

    def bulk(ref, j, count, send_sem, recv_sem):
        part = ref.at[j, pl.ds(0, count)]
        return pltpu.make_async_remote_copy(
            src_ref=part, dst_ref=part, send_sem=send_sem, recv_sem=recv_sem,
            device_id=(me,), device_id_type=MESH,
        )

    def row_code(q, h, shape, dim):
        r = iota(shape, dim)
        a, b, low = r >> 6, (r >> 4) & 3, r & 15
        core = c if h == 0 else other
        return (plane_peer(q, a, b, core) * 16 + low).astype(jnp.float32)

    def line_aux(q):
        group = iota((8, 128), 1) >> 5
        found = jnp.zeros((8, 128), jnp.float32)
        for s in range(LINE):
            found = jnp.where(group == s, aux[q, s], found)
        return found + jnp.where(iota((8, 128), 0) < 4, (group * 4).astype(jnp.float32), 0.0)

    for q in range(KINDS):
        bulk(aux, q, LINE - 1, sa.at[q], ra.at[q]).wait_recv()
    found = [line_aux(q) for q in range(KINDS)]
    for h in range(2):
        for q in range(KINDS):
            want = row_code(q, h, (ROWS, 128), 0)
            hit = found[q][0:1] == want
            for k in range(1, 4):
                hit = hit | (found[q][k:k + 1] == want)
            picks[q, h] = jnp.where(hit, 1.0, 0.0).astype(jnp.bfloat16)

    def exchange(src, dst, h, part, send_sem, recv_sem):
        core = c if h == 0 else other

        def body(t, carry):
            for j in part:
                q = j % 3
                turn = (t * STRIDE[q]) % 16
                a, b = rel(plane[q][0], turn // 4), rel(plane[q][1], turn % 4)
                pltpu.make_async_remote_copy(
                    src_ref=src.at[j, h * 16 + a * 4 + b],
                    dst_ref=dst.at[j, h * 16 + plane[q][0] * 4 + plane[q][1]],
                    send_sem=send_sem.at[h * CHUNKS + j], recv_sem=recv_sem.at[h * CHUNKS + j],
                    device_id=(plane_peer(q, a, b, core),), device_id_type=MESH,
                ).start()
            return carry

        lax.fori_loop(1 - h, 16, body, 0)
        if h == 0:
            for j in part:
                mine = plane[j % 3][0] * 4 + plane[j % 3][1]
                dst[j, pl.ds(mine, 1)] = src[j, pl.ds(mine, 1)]

    for h in range(2):
        for part in PARTS:
            for j in part:
                if h == 0:
                    bulk(xa, j, LINE - 1, s1.at[j], r1.at[j]).wait_recv()
                rows = jnp.dot(
                    picks[j % 3, h], xa[j].reshape(LINE * TOK, CHUNK),
                    preferred_element_type=jnp.float32,
                )
                sb[j, h * 16:(h + 1) * 16] = rows.astype(jnp.bfloat16).reshape(16, 16, CHUNK)
            exchange(sb, rb, h, part, s2, r2)

    for q in range(KINDS):
        cols = jnp.transpose(
            jnp.concatenate([found[q], jnp.zeros((120, 128), jnp.float32)], axis=0)
        )
        for h in range(2):
            want = row_code(q, h, (128, ROWS), 1)
            factor = jnp.zeros((128, ROWS), jnp.float32)
            for k in range(4):
                factor = jnp.where(cols[:, k:k + 1] == want, cols[:, 4 + k:5 + k], factor)
            high = factor.astype(jnp.bfloat16)
            wm_hi[q, h] = high
            wm_lo[q, h] = (factor - high.astype(jnp.float32)).astype(jnp.bfloat16)

    def swap(high, low):
        i, j = iota((ROWS, ROWS), 0), iota((ROWS, ROWS), 1)
        rest = 255 - (3 << high) - (3 << low)
        moved = (i & rest) | (((i >> high) & 3) << low) | (((i >> low) & 3) << high)
        return jnp.where(moved == j, 1.0, 0.0).astype(jnp.bfloat16)

    orders = (None, swap(4, 2), swap(6, 2))

    def in_order(q, rows):
        if q == 0:
            return rows
        return jnp.dot(orders[q], rows, preferred_element_type=jnp.float32).astype(jnp.bfloat16)

    for copy in weights:
        copy.wait()
    for h in range(2):
        for j in range(CHUNKS):
            i = h * CHUNKS + j
            bulk(rb, j, 15 + h, s2.at[i], r2.at[i]).wait_recv()
            rows = rb[j, h * 16:(h + 1) * 16].reshape(ROWS, CHUNK)
            xp[:, columns(j)] = in_order(j % 3, rows)
        acts = jnp.dot(xp[...], w_in[...], preferred_element_type=jnp.float32)
        gate_act, up_act = acts[:, :FFE], acts[:, FFE:]
        hidden = (gate_act * jax.nn.sigmoid(gate_act) * up_act).astype(jnp.bfloat16)
        hidden = [in_order(q, hidden) for q in range(KINDS)]
        for part in PARTS:
            for j in part:
                made = jnp.dot(hidden[j % 3], w_out[:, columns(j)], preferred_element_type=jnp.float32)
                ob[j, h * 16:(h + 1) * 16] = made.astype(jnp.bfloat16).reshape(16, 16, CHUNK)
            exchange(ob, gb, h, part, s3, r3)

    def here(q, j):
        return parts_ref.at[pos[q], :, pl.ds(j * CHUNK, CHUNK)]

    for h in range(2):
        for j in range(CHUNKS):
            q, i = j % 3, h * CHUNKS + j
            bulk(gb, j, 15 + h, s3.at[i], r3.at[i]).wait_recv()
            rows = gb[j, h * 16:(h + 1) * 16].reshape(ROWS, CHUNK)
            part = jnp.dot(wm_hi[q, h], rows, preferred_element_type=jnp.float32)
            part += jnp.dot(wm_lo[q, h], rows, preferred_element_type=jnp.float32)
            if h == 0:
                tsum[j] = part
            else:
                tb[j] = (tsum[j] + part).astype(jnp.bfloat16).reshape(LINE, TOK, CHUNK)
                for step in (2, 1, 3):
                    there = rel(pos[q], step)
                    pltpu.make_async_remote_copy(
                        src_ref=tb.at[j, there], dst_ref=here(q, j),
                        send_sem=s4.at[j], recv_sem=r4.at[j],
                        device_id=(line_peer(q, there, c),), device_id_type=MESH,
                    ).start()
                pltpu.make_async_copy(tb.at[j, pos[q]], here(q, j), own_sem.at[j]).start()

    for j in range(CHUNKS):
        q = j % 3
        bulk(xa, j, LINE - 1, s1.at[j], r1.at[j]).wait_send()
        for h in range(2):
            i = h * CHUNKS + j
            bulk(sb, j, 15 + h, s2.at[i], r2.at[i]).wait_send()
            bulk(ob, j, 15 + h, s3.at[i], r3.at[i]).wait_send()
    for q in range(KINDS):
        bulk(aux, q, LINE - 1, sa.at[q], ra.at[q]).wait_send()
    for j in range(CHUNKS):
        q = j % 3
        pltpu.make_async_copy(tb.at[j, pos[q]], here(q, j), own_sem.at[j]).wait()
        bulk(tb, j, LINE - 1, s4.at[j], r4.at[j]).wait()


def local(
    tokens, norm_gain, expert_ids, expert_scores, group_prob, gate_weight, up_weight, down_weight
):
    hbm = pl.BlockSpec(memory_space=pl.ANY)
    bf16, f32 = jnp.bfloat16, jnp.float32
    dma = pltpu.SemaphoreType.DMA
    width = CHUNKS * CHUNK
    rows = pltpu.VMEM((CHUNKS, 32, 16, CHUNK), bf16)
    line = (CHUNKS, LINE, TOK, CHUNK)
    parts = pl.pallas_call(
        step_kernel,
        out_shape=jax.ShapeDtypeStruct((LINE, TOK, width), bf16),
        in_specs=[hbm] * 8,
        out_specs=hbm,
        scratch_shapes=[
            pltpu.VMEM((TOK, width), bf16),
            pltpu.VMEM((1, width), f32),
            pltpu.VMEM((4, TOK), jnp.int32),
            pltpu.VMEM((4, TOK), f32),
            pltpu.VMEM((1, TOK), f32),
            pltpu.VMEM((8, 128), f32),
            pltpu.VMEM((width, 2 * FFE), bf16),
            pltpu.VMEM((FFE, width), bf16),
            pltpu.VMEM(line, bf16),
            pltpu.VMEM((KINDS, LINE, 8, 128), f32),
            pltpu.VMEM((KINDS, 2, ROWS, 128), bf16),
            rows,
            rows,
            pltpu.VMEM((ROWS, width), bf16),
            rows,
            rows,
            pltpu.VMEM((CHUNKS, LINE * TOK, CHUNK), f32),
            pltpu.VMEM(line, bf16),
            pltpu.VMEM((KINDS, 2, 128, ROWS), bf16),
            pltpu.VMEM((KINDS, 2, 128, ROWS), bf16),
            dma((5,)), dma((3,)), dma((6,)),
            dma((6,)), dma((6,)),
            dma((3,)), dma((3,)),
            dma((12,)), dma((12,)),
            dma((12,)), dma((12,)),
            dma((6,)), dma((6,)),
        ],
        compiler_params=pltpu.CompilerParams(
            collective_id=0, has_side_effects=True, vmem_limit_bytes=60 * 2**20
        ),
        name="expert_step",
    )(
        tokens, norm_gain[None, :], expert_ids.T, expert_scores.T, group_prob[None, :],
        gate_weight, up_weight, down_weight,
    )
    terms = [parts[s].astype(f32) for s in range(LINE)]
    return ((terms[0] + terms[1]) + (terms[2] + terms[3])).astype(bf16)


def solution(mesh):
    in_specs = (
        P("ep", None),
        P(),
        P("ep", None),
        P("ep", None),
        P("ep"),
        P("ep", None, None),
        P("ep", None, None),
        P("ep", None, None),
    )
    out_specs = P("ep", None)
    return jax.shard_map(local, mesh=mesh, in_specs=in_specs, out_specs=out_specs, check_vma=False)
```

```python
import jax
import jax.numpy as jnp
from jax import lax
from jax.experimental import pallas as pl
from jax.experimental.pallas import tpu as pltpu
from jax.sharding import PartitionSpec as P

eps_norm = 1e-05
MESH = pl.DeviceIdType.MESH

LINE = 4
TOK = 32
CHUNK = 1024
CHUNKS = 3
PIECE = 512
PIECES = 6
PARTS = ((0, 1, 2), (3, 4, 5))
ROWS = 256
FFE = 384
STRIDE = (7, 11, 13)
FAR = (10, 9, 6, 11, 14, 8, 2, 5, 7, 13, 15, 4, 1, 12, 3, 0)


def iota(shape, dim):
    return lax.broadcasted_iota(jnp.int32, shape, dim)


def one_hot(hit):
    return jnp.where(hit, 1.0, 0.0).astype(jnp.bfloat16)


def device(z, y, x, c):
    return ((z * 4 + y) * 4 + x) * 2 + c


def columns(j):
    low = (j % 3) * CHUNK + (j // 3) * PIECE
    return slice(low, low + PIECE)


def step_kernel(
    tok_hbm, gain_hbm, ids_hbm, score_hbm, prob_hbm, gate_hbm, up_hbm, down_hbm,
    parts_ref,
    tok_ref, gain_ref, ids_ref, score_ref, prob_ref, spread,
    w_in, w_out, xa, aux, codes, sb, rb, xp, ob, gb, tsum, tb, wm,
    in_sem, w_sem, own_sem, s1, r1, sa, ra, sl, rl, sn, rn, s2, r2, s3, r3, s4, r4,
):
    me = lax.axis_index("ep")
    z, y, x, c = me // 32, (me // 8) % 4, (me // 2) % 4, me % 2
    other = 1 - c
    pos = (x, y, z)
    plane = ((z, y), (z, x), (x, y))

    def rel(value, step):
        return (value + step) % 4

    def line_peer(q, step, core):
        p = rel(pos[q], step)
        return (
            device(z, y, p, core),
            device(z, p, x, core),
            device(p, y, x, core),
        )[q]

    def plane_peer(q, a, b, core):
        return (
            device(a, b, x, core),
            device(a, y, b, core),
            device(z, b, a, core),
        )[q]

    smalls = [
        pltpu.make_async_copy(src, dst, in_sem.at[i])
        for i, (src, dst) in enumerate((
            (tok_hbm, tok_ref), (gain_hbm, gain_ref), (ids_hbm, ids_ref),
            (score_hbm, score_ref), (prob_hbm, prob_ref),
        ))
    ]
    for copy in smalls:
        copy.start()
    weights = [
        pltpu.make_async_copy(gate_hbm.at[0], w_in.at[:, pl.ds(0, FFE)], w_sem.at[0]),
        pltpu.make_async_copy(up_hbm.at[0], w_in.at[:, pl.ds(FFE, FFE)], w_sem.at[1]),
        pltpu.make_async_copy(down_hbm.at[0], w_out, w_sem.at[2]),
    ]
    for copy in weights:
        copy.start()
    barrier = pltpu.get_barrier_semaphore()
    for step in (2, 1, 3):
        for q in range(CHUNKS):
            for core in (c, other):
                pl.semaphore_signal(
                    barrier, inc=1, device_id=(line_peer(q, step, core),), device_id_type=MESH
                )
    pl.semaphore_signal(barrier, inc=1, device_id=(device(z, y, x, other),), device_id_type=MESH)

    for copy in smalls[:2]:
        copy.wait()

    values = tok_ref[...].astype(jnp.float32)
    centred = values - jnp.mean(values, axis=1, keepdims=True)
    variance = jnp.mean(centred * centred, axis=1, keepdims=True)
    normed = (centred * lax.rsqrt(variance + eps_norm) * gain_ref[...]).astype(jnp.bfloat16)
    for q in range(CHUNKS):
        xa[q, 0, 0] = normed[:, q * CHUNK:(q + 1) * CHUNK]

    def send(src, dst, send_sem, recv_sem, peer):
        pltpu.make_async_remote_copy(
            src_ref=src, dst_ref=dst, send_sem=send_sem, recv_sem=recv_sem,
            device_id=(peer,), device_id_type=MESH,
        ).start()

    def to_neighbours(q, d):
        for step in (1, 3):
            send(
                xa.at[q, 0, d], xa.at[q, 4 - step, d], sn.at[q, step, d], rn.at[q, 4 - step, d],
                line_peer((q + 1) % 3, step, c),
            )

    for copy in smalls[2:]:
        copy.wait()
    ids = ids_ref[...]
    scores = score_ref[...]
    exp_scores = jnp.exp(scores - jnp.max(scores, axis=0, keepdims=True))
    mixing = exp_scores / jnp.sum(exp_scores, axis=0, keepdims=True) * prob_ref[...]
    expert = iota((128, TOK), 0)
    matches = [ids[k:k + 1] == expert for k in range(4)]
    named = sum(jnp.where(match, 1.0, 0.0) for match in matches)
    earlier = jnp.where(iota((TOK, TOK), 0) < iota((TOK, TOK), 1), 1.0, 0.0)
    rank = jnp.dot(
        named.astype(jnp.bfloat16), earlier.astype(jnp.bfloat16),
        preferred_element_type=jnp.float32,
    )
    spread[...] = jnp.zeros((8, 128), jnp.float32)
    for k in range(4):
        slot = jnp.sum(jnp.where(matches[k], rank, 0.0), axis=0, keepdims=True)
        spread[k:k + 1, 0:TOK] = ids[k:k + 1].astype(jnp.float32) * 16.0 + slot
        spread[4 + k:5 + k, 0:TOK] = mixing[k:k + 1]
    own = spread[...]
    own = own + pltpu.roll(own, TOK, 1)
    own = own + pltpu.roll(own, 2 * TOK, 1)
    quarter = ((iota((8, 128), 1) >> 5) * 4).astype(jnp.float32)
    own = own + jnp.where(iota((8, 128), 0) < 4, quarter, 0.0)
    for q in range(CHUNKS):
        aux[q, 0] = own

    pl.semaphore_wait(barrier, 19)
    for step in (2, 1, 3):
        for q in range(CHUNKS):
            send(
                aux.at[q, 0], aux.at[q, 4 - step], sa.at[q, step], ra.at[q, 4 - step],
                line_peer(q, step, c),
            )
    for step in (2, 1, 3):
        for q in range(CHUNKS):
            send(
                xa.at[q, 0, 0], xa.at[q, 0, 4 - step], s1.at[q, step], r1.at[q, 4 - step],
                line_peer(q, step, c),
            )
    for q in range(CHUNKS):
        to_neighbours(q, 0)

    def whole(ref, send_sem, recv_sem):
        return pltpu.make_async_remote_copy(
            src_ref=ref, dst_ref=ref, send_sem=send_sem, recv_sem=recv_sem,
            device_id=(me,), device_id_type=MESH,
        )

    def bulk(ref, j, h, low, width, send_sem, recv_sem):
        part = ref.at[j, pl.ds(0, 15 + h), :, pl.ds(low, width)]
        i = (1 + h) if low else h
        return whole(part, send_sem.at[i, j], recv_sem.at[i, j])

    def row_code(q, h, shape, dim):
        r = iota(shape, dim)
        a, b, low = r >> 6, (r >> 4) & 3, r & 15
        core = c if h == 0 else other
        return (plane_peer(q, a, b, core) * 16 + low).astype(jnp.float32)

    def exchange(h, part, low=0, width=PIECE):
        core = c if h == 0 else other

        def body(t, carry):
            for j in part:
                q = j % 3
                turn = t if low else (t * STRIDE[q]) % 16
                a, b = rel(plane[q][0], turn // 4), rel(plane[q][1], turn % 4)
                i = (1 + h) if low else h
                send(
                    ob.at[j, h * 16 + a * 4 + b, :, pl.ds(low, width)],
                    gb.at[j, h * 16 + plane[q][0] * 4 + plane[q][1], :, pl.ds(low, width)],
                    s3.at[i, j], r3.at[i, j], plane_peer(q, a, b, core),
                )
            return carry

        if low:
            for t in FAR:
                body(t, 0)
        else:
            lax.fori_loop(1 - h, 16, body, 0)
        if h == 0:
            for j in part:
                mine = plane[j % 3][0] * 4 + plane[j % 3][1]
                gb[j, pl.ds(mine, 1)] = ob[j, pl.ds(mine, 1)]

    for q in range(CHUNKS):
        for d in (1, 3, 2):
            whole(aux.at[q, d], sa.at[q, d], ra.at[q, d]).wait_recv()
    group = iota((8, 128), 1) >> 5
    for q in range(CHUNKS):
        found = aux[q, 0]
        for d in range(1, LINE):
            found = jnp.where(group == d, aux[q, d], found)
        codes[q, 0] = found
    for step in (2, 1, 3):
        for q in range(CHUNKS):
            send(
                codes.at[q, 0], codes.at[q, 4 - step], sl.at[q, step], rl.at[q, 4 - step],
                line_peer((q + 1) % 3, step, c),
            )
    for d in (1, 3, 2):
        for q in range(CHUNKS):
            whole(xa.at[q, 0, d], s1.at[q, d], r1.at[q, d]).wait_recv()
            to_neighbours(q, d)

    half = CHUNK // 2

    def select(e):
        for q in range(CHUNKS):
            r = iota((128, 128), 0)
            h, step = r >> 6, (r >> 4) & 3
            core = c + h - 2 * c * h
            want = (line_peer((q + 2) % 3, step, core) * 16 + (r & 15)).astype(jnp.float32)
            found = codes[q, e]
            hit = found[0:1] == want
            for k in range(1, 4):
                hit = hit | (found[k:k + 1] == want)
            rows = jnp.dot(
                one_hot(hit), xa[q, e].reshape(LINE * TOK, CHUNK),
                preferred_element_type=jnp.float32,
            )
            sb[q, e] = rows.astype(jnp.bfloat16).reshape(2, LINE, 16, CHUNK)

    def deliver(h, e):
        core = c if h == 0 else other
        for step in (2, 1, 3, 0):
            for q in range(CHUNKS):
                if h == 0 and step == 0:
                    rb[q, 0, 0, e] = sb[q, e, 0, 0]
                    continue
                for low in (0, half):
                    send(
                        sb.at[q, e, h, step, :, pl.ds(low, half)],
                        rb.at[q, h, (4 - step) % 4, e, :, pl.ds(low, half)],
                        s2.at[q, h], r2.at[q, h], line_peer((q + 2) % 3, step, core),
                    )

    select(0)
    deliver(0, 0)
    for d in (0, 1, 3, 2):
        for q in range(CHUNKS):
            for step, low in ((3, 0), (1, half)):
                e = 4 - step
                whole(xa.at[q, e, d], sn.at[q, e, d], rn.at[q, e, d]).wait_recv()
                send(
                    xa.at[q, e, d, :, pl.ds(low, half)], xa.at[q, 2, d, :, pl.ds(low, half)],
                    sn.at[q, 2, 0], rn.at[q, 2, 0], line_peer((q + 1) % 3, step, c),
                )
    for q in range(CHUNKS):
        for e in (1, 3, 2):
            whole(codes.at[q, e], sl.at[q, e], rl.at[q, e]).wait_recv()
    for e in (1, 3):
        select(e)
        deliver(0, e)
    for q in range(CHUNKS):
        whole(xa.at[q, 2], sn.at[q, 2, 0], rn.at[q, 2, 0]).wait_recv()
    select(2)
    deliver(0, 2)
    for e in (0, 1, 3, 2):
        deliver(1, e)

    for q in range(CHUNKS):
        cols = jnp.transpose(
            jnp.concatenate([codes[q, 0], jnp.zeros((120, 128), jnp.float32)], axis=0)
        )
        for h in range(2):
            want = row_code(q, h, (128, ROWS), 1)
            factor = jnp.zeros((128, ROWS), jnp.float32)
            for k in range(4):
                factor = jnp.where(cols[:, k:k + 1] == want, cols[:, 4 + k:5 + k], factor)
            high = factor.astype(jnp.bfloat16)
            wm[q, h, 0:128] = high
            wm[q, h, 128:256] = (factor - high.astype(jnp.float32)).astype(jnp.bfloat16)

    square = (ROWS, ROWS)

    def arrived(q, o):
        zz, yy, xx, slot = o >> 6, (o >> 4) & 3, (o >> 2) & 3, o & 3
        if q == 1:
            return xx * 64 + zz * 16 + yy * 4 + slot
        return yy * 64 + xx * 16 + zz * 4 + slot

    def leaving(q, o):
        zz, yy, xx, slot = o >> 6, (o >> 4) & 3, (o >> 2) & 3, o & 3
        az, ay, ax = (zz + z) & 3, (yy + y) & 3, (xx + x) & 3
        if q == 0:
            return az * 64 + ay * 16 + xx * 4 + slot
        if q == 1:
            return az * 64 + ax * 16 + yy * 4 + slot
        return ax * 64 + ay * 16 + zz * 4 + slot

    gather_order = [None] + [
        one_hot(arrived(q, iota(square, 0)) == iota(square, 1)) for q in (1, 2)
    ]
    spread_order = [
        one_hot(leaving(q, iota(square, 1)) == iota(square, 0)) for q in range(CHUNKS)
    ]

    def ordered(order, rows):
        if order is None:
            return rows
        return jnp.dot(order, rows, preferred_element_type=jnp.float32).astype(jnp.bfloat16)

    for copy in weights:
        copy.wait()
    for h in range(2):
        for q in range(CHUNKS):
            part = rb.at[q, h] if h else rb.at[q, 0, pl.ds(0, 3)]
            whole(part, s2.at[q, h], r2.at[q, h]).wait_recv()
            rows = rb[q, h].reshape(ROWS, CHUNK)
            xp[:, q * CHUNK:(q + 1) * CHUNK] = ordered(gather_order[q], rows)
        acts = jnp.dot(xp[...], w_in[...], preferred_element_type=jnp.float32)
        gate_act, up_act = acts[:, :FFE], acts[:, FFE:]
        hidden = (gate_act * jax.nn.sigmoid(gate_act) * up_act).astype(jnp.bfloat16)
        hidden = [ordered(spread_order[q], hidden) for q in range(CHUNKS)]
        for part in PARTS:
            for j in part:
                made = jnp.dot(
                    hidden[j % 3], w_out[:, columns(j)], preferred_element_type=jnp.float32
                )
                ob[j, h * 16:(h + 1) * 16] = made.astype(jnp.bfloat16).reshape(16, 16, PIECE)
            if h == 1 and part is PARTS[1]:
                exchange(1, part, 0, PIECE // 2)
                exchange(1, part, PIECE // 2, PIECE // 2)
            else:
                exchange(h, part)

    def here(j, slot, low, width):
        return parts_ref.at[slot, :, pl.ds(columns(j).start + low, width)]

    def summed(j, h, low, width):
        bulk(gb, j, h, low, width, s3, r3).wait_recv()
        rows = gb[j, h * 16:(h + 1) * 16, :, low:low + width].reshape(ROWS, width)
        both = jnp.dot(wm[j % 3, h], rows, preferred_element_type=jnp.float32)
        return both[0:128] + both[128:256]

    def settle(j, low, width):
        q = j % 3
        total = tsum[j, :, low:low + width] + summed(j, 1, low, width)
        tb[j, :, :, low:low + width] = total.astype(jnp.bfloat16).reshape(LINE, TOK, width)
        i = 1 if low else 0
        for d in (2, 1, 3):
            send(
                tb.at[j, d, :, pl.ds(low, width)], here(j, 4 - d, low, width),
                s4.at[i, j], r4.at[i, j], line_peer(q, d, c),
            )
        pltpu.make_async_copy(
            tb.at[j, 0, :, pl.ds(low, width)], here(j, 0, low, width), own_sem.at[i, j]
        ).start()

    settles = [(j, 0, PIECE) for j in PARTS[0]]
    settles += [(j, 0, PIECE // 2) for j in PARTS[1]]
    settles += [(j, PIECE // 2, PIECE // 2) for j in PARTS[1]]
    for j in range(PIECES):
        tsum[j] = summed(j, 0, 0, PIECE)
    for j, low, width in settles:
        settle(j, low, width)

    for q in range(CHUNKS):
        for d in range(LINE):
            if d > 0:
                whole(aux.at[q, d], sa.at[q, d], ra.at[q, d]).wait_send()
                whole(codes.at[q, d], sl.at[q, d], rl.at[q, d]).wait_send()
                whole(xa.at[q, 0, d], s1.at[q, d], r1.at[q, d]).wait_send()
            for e in (1, 3):
                whole(xa.at[q, e, d], sn.at[q, e, d], rn.at[q, e, d]).wait_send()
        whole(xa.at[q, 2], sn.at[q, 2, 0], rn.at[q, 2, 0]).wait_send()
        for h in range(2):
            part = rb.at[q, h] if h else rb.at[q, 0, pl.ds(0, 3)]
            whole(part, s2.at[q, h], r2.at[q, h]).wait_send()
    for j in range(PIECES):
        bulk(ob, j, 0, 0, PIECE, s3, r3).wait_send()
    for j, low, width in settles:
        i = 1 if low else 0
        bulk(ob, j, 1, low, width, s3, r3).wait_send()
        part = tb.at[j, pl.ds(0, 3), :, pl.ds(low, width)]
        whole(part, s4.at[i, j], r4.at[i, j]).wait()
        pltpu.make_async_copy(
            tb.at[j, 0, :, pl.ds(low, width)], here(j, 0, low, width), own_sem.at[i, j]
        ).wait()


def local(
    tokens, norm_gain, expert_ids, expert_scores, group_prob, gate_weight, up_weight, down_weight
):
    hbm = pl.BlockSpec(memory_space=pl.ANY)
    bf16, f32 = jnp.bfloat16, jnp.float32
    dma = pltpu.SemaphoreType.DMA
    width = CHUNKS * CHUNK
    rows = pltpu.VMEM((PIECES, 32, 16, PIECE), bf16)
    line = (CHUNKS, LINE)
    parts = pl.pallas_call(
        step_kernel,
        out_shape=jax.ShapeDtypeStruct((LINE, TOK, width), bf16),
        in_specs=[hbm] * 8,
        out_specs=hbm,
        scratch_shapes=[
            pltpu.VMEM((TOK, width), bf16),
            pltpu.VMEM((1, width), f32),
            pltpu.VMEM((4, TOK), jnp.int32),
            pltpu.VMEM((4, TOK), f32),
            pltpu.VMEM((1, TOK), f32),
            pltpu.VMEM((8, 128), f32),
            pltpu.VMEM((width, 2 * FFE), bf16),
            pltpu.VMEM((FFE, width), bf16),
            pltpu.VMEM(line + (LINE, TOK, CHUNK), bf16),
            pltpu.VMEM(line + (8, 128), f32),
            pltpu.VMEM(line + (8, 128), f32),
            pltpu.VMEM(line + (2, LINE, 16, CHUNK), bf16),
            pltpu.VMEM((CHUNKS, 2, LINE, LINE, 16, CHUNK), bf16),
            pltpu.VMEM((ROWS, width), bf16),
            rows,
            rows,
            pltpu.VMEM((PIECES, LINE * TOK, PIECE), f32),
            pltpu.VMEM((PIECES, LINE, TOK, PIECE), bf16),
            pltpu.VMEM((CHUNKS, 2, 256, ROWS), bf16),
            dma((5,)), dma((3,)), dma((2, PIECES)),
            dma(line), dma(line),
            dma(line), dma(line),
            dma(line), dma(line),
            dma(line + (LINE,)), dma(line + (LINE,)),
            dma((CHUNKS, 2)), dma((CHUNKS, 2)),
            dma((3, PIECES)), dma((3, PIECES)),
            dma((2, PIECES)), dma((2, PIECES)),
        ],
        compiler_params=pltpu.CompilerParams(
            collective_id=0, has_side_effects=True, vmem_limit_bytes=60 * 2**20
        ),
        name="expert_step",
    )(
        tokens, norm_gain[None, :], expert_ids.T, expert_scores.T, group_prob[None, :],
        gate_weight, up_weight, down_weight,
    )
    terms = [parts[s].astype(f32) for s in range(LINE)]
    return ((terms[0] + terms[1]) + (terms[2] + terms[3])).astype(bf16)


def solution(mesh):
    in_specs = (
        P("ep", None),
        P(),
        P("ep", None),
        P("ep", None),
        P("ep"),
        P("ep", None, None),
        P("ep", None, None),
        P("ep", None, None),
    )
    out_specs = P("ep", None)
    return jax.shard_map(local, mesh=mesh, in_specs=in_specs, out_specs=out_specs, check_vma=False)
```

```python
import jax
import jax.numpy as jnp
from jax import lax
from jax.experimental import pallas as pl
from jax.experimental.pallas import tpu as pltpu
from jax.sharding import PartitionSpec as P

eps_norm = 1e-05
MESH = pl.DeviceIdType.MESH

LINE = 4
TOK = 32
CHUNK = 1024
CHUNKS = 3
PIECE = 256
PIECES = 12
PARTS = ((0, 1, 2), (3, 4, 5), (6, 7, 8), (9, 10, 11))
ROWS = 256
FFE = 384
STRIDE = (7, 11, 13)
FAR = (10, 9, 6, 11, 14, 8, 2, 5, 7, 13, 15, 4, 1, 12, 3, 0)


def iota(shape, dim):
    return lax.broadcasted_iota(jnp.int32, shape, dim)


def one_hot(hit):
    return jnp.where(hit, 1.0, 0.0).astype(jnp.bfloat16)


def device(z, y, x, c):
    return ((z * 4 + y) * 4 + x) * 2 + c


def columns(j):
    low = (j % 3) * CHUNK + (j // 3) * PIECE
    return slice(low, low + PIECE)


def step_kernel(
    tok_hbm, gain_hbm, ids_hbm, score_hbm, prob_hbm, gate_hbm, up_hbm, down_hbm,
    parts_ref,
    tok_ref, gain_ref, ids_ref, score_ref, prob_ref, spread,
    w_in, w_out, xa, aux, codes, sb, rb, xp, ob, gb, tsum, tb, wm,
    in_sem, w_sem, own_sem, s1, r1, sa, ra, sl, rl, sn, rn, s2, r2, s3, r3, s4, r4,
):
    me = lax.axis_index("ep")
    z, y, x, c = me // 32, (me // 8) % 4, (me // 2) % 4, me % 2
    other = 1 - c
    pos = (x, y, z)
    plane = ((z, y), (z, x), (x, y))

    def rel(value, step):
        return (value + step) % 4

    def line_peer(q, step, core):
        p = rel(pos[q], step)
        return (
            device(z, y, p, core),
            device(z, p, x, core),
            device(p, y, x, core),
        )[q]

    def plane_peer(q, a, b, core):
        return (
            device(a, b, x, core),
            device(a, y, b, core),
            device(z, b, a, core),
        )[q]

    smalls = [
        pltpu.make_async_copy(src, dst, in_sem.at[i])
        for i, (src, dst) in enumerate((
            (tok_hbm, tok_ref), (gain_hbm, gain_ref), (ids_hbm, ids_ref),
            (score_hbm, score_ref), (prob_hbm, prob_ref),
        ))
    ]
    for copy in smalls:
        copy.start()
    weights = [
        pltpu.make_async_copy(gate_hbm.at[0], w_in.at[:, pl.ds(0, FFE)], w_sem.at[0]),
        pltpu.make_async_copy(up_hbm.at[0], w_in.at[:, pl.ds(FFE, FFE)], w_sem.at[1]),
        pltpu.make_async_copy(down_hbm.at[0], w_out, w_sem.at[2]),
    ]
    for copy in weights:
        copy.start()
    barrier = pltpu.get_barrier_semaphore()
    for step in (2, 1, 3):
        for q in range(CHUNKS):
            for core in (c, other):
                pl.semaphore_signal(
                    barrier, inc=1, device_id=(line_peer(q, step, core),), device_id_type=MESH
                )
    pl.semaphore_signal(barrier, inc=1, device_id=(device(z, y, x, other),), device_id_type=MESH)

    for copy in smalls:
        copy.wait()

    values = tok_ref[...].astype(jnp.float32)
    centred = values - jnp.mean(values, axis=1, keepdims=True)
    variance = jnp.mean(centred * centred, axis=1, keepdims=True)
    normed = (centred * lax.rsqrt(variance + eps_norm) * gain_ref[...]).astype(jnp.bfloat16)
    for q in range(CHUNKS):
        xa[q, 0, 0] = normed[:, q * CHUNK:(q + 1) * CHUNK]

    def send(src, dst, send_sem, recv_sem, peer):
        pltpu.make_async_remote_copy(
            src_ref=src, dst_ref=dst, send_sem=send_sem, recv_sem=recv_sem,
            device_id=(peer,), device_id_type=MESH,
        ).start()

    def to_neighbours(q, d):
        for step in (1, 3):
            send(
                xa.at[q, 0, d], xa.at[q, 4 - step, d], sn.at[q, step, d], rn.at[q, 4 - step, d],
                line_peer((q + 1) % 3, step, c),
            )

    ids = ids_ref[...]
    scores = score_ref[...]
    exp_scores = jnp.exp(scores - jnp.max(scores, axis=0, keepdims=True))
    mixing = exp_scores / jnp.sum(exp_scores, axis=0, keepdims=True) * prob_ref[...]
    expert = iota((128, TOK), 0)
    matches = [ids[k:k + 1] == expert for k in range(4)]
    named = sum(jnp.where(match, 1.0, 0.0) for match in matches)
    earlier = jnp.where(iota((TOK, TOK), 0) < iota((TOK, TOK), 1), 1.0, 0.0)
    rank = jnp.dot(
        named.astype(jnp.bfloat16), earlier.astype(jnp.bfloat16),
        preferred_element_type=jnp.float32,
    )
    spread[...] = jnp.zeros((8, 128), jnp.float32)
    for k in range(4):
        slot = jnp.sum(jnp.where(matches[k], rank, 0.0), axis=0, keepdims=True)
        spread[k:k + 1, 0:TOK] = ids[k:k + 1].astype(jnp.float32) * 16.0 + slot
        spread[4 + k:5 + k, 0:TOK] = mixing[k:k + 1]
    own = spread[...]
    own = own + pltpu.roll(own, TOK, 1)
    own = own + pltpu.roll(own, 2 * TOK, 1)
    quarter = ((iota((8, 128), 1) >> 5) * 4).astype(jnp.float32)
    own = own + jnp.where(iota((8, 128), 0) < 4, quarter, 0.0)
    for q in range(CHUNKS):
        aux[q, 0] = own

    pl.semaphore_wait(barrier, 19)
    for step in (2, 1, 3):
        for q in range(CHUNKS):
            send(
                aux.at[q, 0], aux.at[q, 4 - step], sa.at[q, step], ra.at[q, 4 - step],
                line_peer(q, step, c),
            )
    for step in (2, 1, 3):
        for q in range(CHUNKS):
            send(
                xa.at[q, 0, 0], xa.at[q, 0, 4 - step], s1.at[q, step], r1.at[q, 4 - step],
                line_peer(q, step, c),
            )
    for q in range(CHUNKS):
        to_neighbours(q, 0)

    def whole(ref, send_sem, recv_sem):
        return pltpu.make_async_remote_copy(
            src_ref=ref, dst_ref=ref, send_sem=send_sem, recv_sem=recv_sem,
            device_id=(me,), device_id_type=MESH,
        )

    def bulk(ref, j, h, send_sem, recv_sem):
        return whole(ref.at[j, pl.ds(0, 15 + h)], send_sem.at[h, j], recv_sem.at[h, j])

    def row_code(q, h, shape, dim):
        r = iota(shape, dim)
        a, b, low = r >> 6, (r >> 4) & 3, r & 15
        core = c if h == 0 else other
        return (plane_peer(q, a, b, core) * 16 + low).astype(jnp.float32)

    def exchange(h, part):
        core = c if h == 0 else other
        last = h == 1 and part is PARTS[-1]

        def body(t, carry):
            for j in part:
                q = j % 3
                turn = t if last else (t * STRIDE[q]) % 16
                a, b = rel(plane[q][0], turn // 4), rel(plane[q][1], turn % 4)
                send(
                    ob.at[j, h * 16 + a * 4 + b],
                    gb.at[j, h * 16 + plane[q][0] * 4 + plane[q][1]],
                    s3.at[h, j], r3.at[h, j], plane_peer(q, a, b, core),
                )
            return carry

        if last:
            for t in FAR:
                body(t, 0)
        else:
            lax.fori_loop(1 - h, 16, body, 0)
        if h == 0:
            for j in part:
                mine = plane[j % 3][0] * 4 + plane[j % 3][1]
                gb[j, pl.ds(mine, 1)] = ob[j, pl.ds(mine, 1)]

    for q in range(CHUNKS):
        for d in (1, 3, 2):
            whole(aux.at[q, d], sa.at[q, d], ra.at[q, d]).wait_recv()
    group = iota((8, 128), 1) >> 5
    for q in range(CHUNKS):
        found = aux[q, 0]
        for d in range(1, LINE):
            found = jnp.where(group == d, aux[q, d], found)
        codes[q, 0] = found
    for step in (2, 1, 3):
        for q in range(CHUNKS):
            send(
                codes.at[q, 0], codes.at[q, 4 - step], sl.at[q, step], rl.at[q, 4 - step],
                line_peer((q + 1) % 3, step, c),
            )
    for d in (1, 3, 2):
        for q in range(CHUNKS):
            whole(xa.at[q, 0, d], s1.at[q, d], r1.at[q, d]).wait_recv()
            to_neighbours(q, d)

    half = CHUNK // 2

    def select(e):
        for q in range(CHUNKS):
            r = iota((128, 128), 0)
            h, step = r >> 6, (r >> 4) & 3
            core = c + h - 2 * c * h
            want = (line_peer((q + 2) % 3, step, core) * 16 + (r & 15)).astype(jnp.float32)
            found = codes[q, e]
            hit = found[0:1] == want
            for k in range(1, 4):
                hit = hit | (found[k:k + 1] == want)
            rows = jnp.dot(
                one_hot(hit), xa[q, e].reshape(LINE * TOK, CHUNK),
                preferred_element_type=jnp.float32,
            )
            sb[q, e] = rows.astype(jnp.bfloat16).reshape(2, LINE, 16, CHUNK)

    def deliver(h, e):
        core = c if h == 0 else other
        for step in (2, 1, 3, 0):
            for q in range(CHUNKS):
                if h == 0 and step == 0:
                    rb[q, 0, 0, e] = sb[q, e, 0, 0]
                    continue
                for low in (0, half):
                    send(
                        sb.at[q, e, h, step, :, pl.ds(low, half)],
                        rb.at[q, h, (4 - step) % 4, e, :, pl.ds(low, half)],
                        s2.at[q, h], r2.at[q, h], line_peer((q + 2) % 3, step, core),
                    )

    for d in (0,):
        for q in range(CHUNKS):
            for step, low in ((3, 0), (1, half)):
                e = 4 - step
                whole(xa.at[q, e, d], sn.at[q, e, d], rn.at[q, e, d]).wait_recv()
                send(
                    xa.at[q, e, d, :, pl.ds(low, half)], xa.at[q, 2, d, :, pl.ds(low, half)],
                    sn.at[q, 2, 0], rn.at[q, 2, 0], line_peer((q + 1) % 3, step, c),
                )
    select(0)
    deliver(0, 0)
    for d in (1, 3, 2):
        for q in range(CHUNKS):
            for step, low in ((3, 0), (1, half)):
                e = 4 - step
                whole(xa.at[q, e, d], sn.at[q, e, d], rn.at[q, e, d]).wait_recv()
                send(
                    xa.at[q, e, d, :, pl.ds(low, half)], xa.at[q, 2, d, :, pl.ds(low, half)],
                    sn.at[q, 2, 0], rn.at[q, 2, 0], line_peer((q + 1) % 3, step, c),
                )
    for q in range(CHUNKS):
        for e in (1, 3, 2):
            whole(codes.at[q, e], sl.at[q, e], rl.at[q, e]).wait_recv()
    for e in (1, 3):
        select(e)
        deliver(0, e)
    for q in range(CHUNKS):
        whole(xa.at[q, 2], sn.at[q, 2, 0], rn.at[q, 2, 0]).wait_recv()
    select(2)
    deliver(0, 2)
    for e in (0, 1, 3, 2):
        deliver(1, e)

    for q in range(CHUNKS):
        cols = jnp.transpose(
            jnp.concatenate([codes[q, 0], jnp.zeros((120, 128), jnp.float32)], axis=0)
        )
        for h in range(2):
            want = row_code(q, h, (128, ROWS), 1)
            factor = jnp.zeros((128, ROWS), jnp.float32)
            for k in range(4):
                factor = jnp.where(cols[:, k:k + 1] == want, cols[:, 4 + k:5 + k], factor)
            high = factor.astype(jnp.bfloat16)
            wm[q, h, 0:128] = high
            wm[q, h, 128:256] = (factor - high.astype(jnp.float32)).astype(jnp.bfloat16)

    square = (ROWS, ROWS)

    def arrived(q, o):
        zz, yy, xx, slot = o >> 6, (o >> 4) & 3, (o >> 2) & 3, o & 3
        if q == 1:
            return xx * 64 + zz * 16 + yy * 4 + slot
        return yy * 64 + xx * 16 + zz * 4 + slot

    def leaving(q, o):
        zz, yy, xx, slot = o >> 6, (o >> 4) & 3, (o >> 2) & 3, o & 3
        az, ay, ax = (zz + z) & 3, (yy + y) & 3, (xx + x) & 3
        if q == 0:
            return az * 64 + ay * 16 + xx * 4 + slot
        if q == 1:
            return az * 64 + ax * 16 + yy * 4 + slot
        return ax * 64 + ay * 16 + zz * 4 + slot

    gather_order = [None] + [
        one_hot(arrived(q, iota(square, 0)) == iota(square, 1)) for q in (1, 2)
    ]
    spread_order = [
        one_hot(leaving(q, iota(square, 1)) == iota(square, 0)) for q in range(CHUNKS)
    ]

    def ordered(order, rows):
        if order is None:
            return rows
        return jnp.dot(order, rows, preferred_element_type=jnp.float32).astype(jnp.bfloat16)

    for copy in weights:
        copy.wait()
    for h in range(2):
        for q in range(CHUNKS):
            part = rb.at[q, h] if h else rb.at[q, 0, pl.ds(0, 3)]
            whole(part, s2.at[q, h], r2.at[q, h]).wait_recv()
            rows = rb[q, h].reshape(ROWS, CHUNK)
            xp[:, q * CHUNK:(q + 1) * CHUNK] = ordered(gather_order[q], rows)
        acts = jnp.dot(xp[...], w_in[...], preferred_element_type=jnp.float32)
        gate_act, up_act = acts[:, :FFE], acts[:, FFE:]
        hidden = (gate_act * jax.nn.sigmoid(gate_act) * up_act).astype(jnp.bfloat16)
        hidden = [ordered(spread_order[q], hidden) for q in range(CHUNKS)]
        for part in PARTS:
            for j in part:
                made = jnp.dot(
                    hidden[j % 3], w_out[:, columns(j)], preferred_element_type=jnp.float32
                )
                ob[j, h * 16:(h + 1) * 16] = made.astype(jnp.bfloat16).reshape(16, 16, PIECE)
            exchange(h, part)

    def here(j, slot):
        return parts_ref.at[slot, :, pl.ds(columns(j).start, PIECE)]

    def summed(j, h):
        rows = gb[j, h * 16:(h + 1) * 16].reshape(ROWS, PIECE)
        both = jnp.dot(wm[j % 3, h], rows, preferred_element_type=jnp.float32)
        return both[0:128] + both[128:256]

    for part in PARTS:
        for j in part:
            bulk(gb, j, 0, s3, r3).wait_recv()
        for j in part:
            tsum[j] = summed(j, 0)
    for part in PARTS:
        for j in part:
            bulk(gb, j, 1, s3, r3).wait_recv()
        for j in part:
            total = tsum[j] + summed(j, 1)
            tb[j] = total.astype(jnp.bfloat16).reshape(LINE, TOK, PIECE)
        for d in (2, 1, 3):
            for j in part:
                send(
                    tb.at[j, d], here(j, 4 - d), s4.at[j], r4.at[j], line_peer(j % 3, d, c)
                )
        for j in part:
            pltpu.make_async_copy(tb.at[j, 0], here(j, 0), own_sem.at[j]).start()

    for q in range(CHUNKS):
        for d in range(LINE):
            if d > 0:
                whole(aux.at[q, d], sa.at[q, d], ra.at[q, d]).wait_send()
                whole(codes.at[q, d], sl.at[q, d], rl.at[q, d]).wait_send()
                whole(xa.at[q, 0, d], s1.at[q, d], r1.at[q, d]).wait_send()
            for e in (1, 3):
                whole(xa.at[q, e, d], sn.at[q, e, d], rn.at[q, e, d]).wait_send()
        whole(xa.at[q, 2], sn.at[q, 2, 0], rn.at[q, 2, 0]).wait_send()
        for h in range(2):
            part = rb.at[q, h] if h else rb.at[q, 0, pl.ds(0, 3)]
            whole(part, s2.at[q, h], r2.at[q, h]).wait_send()
    for j in range(PIECES):
        for h in range(2):
            bulk(ob, j, h, s3, r3).wait_send()
        whole(tb.at[j, pl.ds(0, 3)], s4.at[j], r4.at[j]).wait()
        pltpu.make_async_copy(tb.at[j, 0], here(j, 0), own_sem.at[j]).wait()


def local(
    tokens, norm_gain, expert_ids, expert_scores, group_prob, gate_weight, up_weight, down_weight
):
    hbm = pl.BlockSpec(memory_space=pl.ANY)
    bf16, f32 = jnp.bfloat16, jnp.float32
    dma = pltpu.SemaphoreType.DMA
    width = CHUNKS * CHUNK
    rows = pltpu.VMEM((PIECES, 32, 16, PIECE), bf16)
    line = (CHUNKS, LINE)
    parts = pl.pallas_call(
        step_kernel,
        out_shape=jax.ShapeDtypeStruct((LINE, TOK, width), bf16),
        in_specs=[hbm] * 8,
        out_specs=hbm,
        scratch_shapes=[
            pltpu.VMEM((TOK, width), bf16),
            pltpu.VMEM((1, width), f32),
            pltpu.VMEM((4, TOK), jnp.int32),
            pltpu.VMEM((4, TOK), f32),
            pltpu.VMEM((1, TOK), f32),
            pltpu.VMEM((8, 128), f32),
            pltpu.VMEM((width, 2 * FFE), bf16),
            pltpu.VMEM((FFE, width), bf16),
            pltpu.VMEM(line + (LINE, TOK, CHUNK), bf16),
            pltpu.VMEM(line + (8, 128), f32),
            pltpu.VMEM(line + (8, 128), f32),
            pltpu.VMEM(line + (2, LINE, 16, CHUNK), bf16),
            pltpu.VMEM((CHUNKS, 2, LINE, LINE, 16, CHUNK), bf16),
            pltpu.VMEM((ROWS, width), bf16),
            rows,
            rows,
            pltpu.VMEM((PIECES, LINE * TOK, PIECE), f32),
            pltpu.VMEM((PIECES, LINE, TOK, PIECE), bf16),
            pltpu.VMEM((CHUNKS, 2, 256, ROWS), bf16),
            dma((5,)), dma((3,)), dma((PIECES,)),
            dma(line), dma(line),
            dma(line), dma(line),
            dma(line), dma(line),
            dma(line + (LINE,)), dma(line + (LINE,)),
            dma((CHUNKS, 2)), dma((CHUNKS, 2)),
            dma((2, PIECES)), dma((2, PIECES)),
            dma((PIECES,)), dma((PIECES,)),
        ],
        compiler_params=pltpu.CompilerParams(
            collective_id=0, has_side_effects=True, vmem_limit_bytes=60 * 2**20
        ),
        name="expert_step",
    )(
        tokens, norm_gain[None, :], expert_ids.T, expert_scores.T, group_prob[None, :],
        gate_weight, up_weight, down_weight,
    )
    terms = [parts[s].astype(f32) for s in range(LINE)]
    return ((terms[0] + terms[1]) + (terms[2] + terms[3])).astype(bf16)


def solution(mesh):
    in_specs = (
        P("ep", None),
        P(),
        P("ep", None),
        P("ep", None),
        P("ep"),
        P("ep", None, None),
        P("ep", None, None),
        P("ep", None, None),
    )
    out_specs = P("ep", None)
    return jax.shard_map(local, mesh=mesh, in_specs=in_specs, out_specs=out_specs, check_vma=False)
```

```python
import jax
import jax.numpy as jnp
from jax import lax
from jax.experimental import pallas as pl
from jax.experimental.pallas import tpu as pltpu
from jax.sharding import PartitionSpec as P

eps_norm = 1e-05
MESH = pl.DeviceIdType.MESH

LINE = 4
TOK = 32
CHUNK = 1024
CHUNKS = 3
PIECE = 256
PIECES = 12
PARTS = ((0, 1, 2), (3, 4, 5), (6, 7, 8), (9, 10, 11))
ROWS = 256
FFE = 384
STRIDE = (7, 11, 13)
FAR = (10, 9, 6, 11, 14, 8, 2, 5, 7, 13, 15, 4, 1, 12, 3, 0)


def iota(shape, dim):
    return lax.broadcasted_iota(jnp.int32, shape, dim)


def one_hot(hit):
    return jnp.where(hit, 1.0, 0.0).astype(jnp.bfloat16)


def device(z, y, x, c):
    return ((z * 4 + y) * 4 + x) * 2 + c


def columns(j):
    low = (j % 3) * CHUNK + (j // 3) * PIECE
    return slice(low, low + PIECE)


def step_kernel(
    tok_hbm, gain_hbm, ids_hbm, score_hbm, prob_hbm, gate_hbm, up_hbm, down_hbm,
    parts_ref,
    tok_ref, gain_ref, ids_ref, score_ref, prob_ref, spread,
    w_in, w_out, xa, aux, codes, sb, rb, xp, ob, gb, tsum, tb, wm,
    in_sem, w_sem, own_sem, s1, r1, sa, ra, sl, rl, sn, rn, s2, r2, s3, r3, s4, r4,
):
    me = lax.axis_index("ep")
    z, y, x, c = me // 32, (me // 8) % 4, (me // 2) % 4, me % 2
    other = 1 - c
    pos = (x, y, z)
    plane = ((z, y), (z, x), (x, y))

    def rel(value, step):
        return (value + step) % 4

    def line_peer(q, step, core):
        p = rel(pos[q], step)
        return (
            device(z, y, p, core),
            device(z, p, x, core),
            device(p, y, x, core),
        )[q]

    def plane_peer(q, a, b, core):
        return (
            device(a, b, x, core),
            device(a, y, b, core),
            device(z, b, a, core),
        )[q]

    barrier = pltpu.get_barrier_semaphore()
    for step in (2, 1, 3):
        for q in range(CHUNKS):
            for core in (c, other):
                pl.semaphore_signal(
                    barrier, inc=1, device_id=(line_peer(q, step, core),), device_id_type=MESH
                )
    pl.semaphore_signal(barrier, inc=1, device_id=(device(z, y, x, other),), device_id_type=MESH)

    smalls = [
        pltpu.make_async_copy(src, dst, in_sem.at[i])
        for i, (src, dst) in enumerate((
            (tok_hbm, tok_ref), (gain_hbm, gain_ref), (ids_hbm, ids_ref),
            (score_hbm, score_ref), (prob_hbm, prob_ref),
        ))
    ]
    for copy in smalls:
        copy.start()
    weights = [
        pltpu.make_async_copy(gate_hbm.at[0], w_in.at[:, pl.ds(0, FFE)], w_sem.at[0]),
        pltpu.make_async_copy(up_hbm.at[0], w_in.at[:, pl.ds(FFE, FFE)], w_sem.at[1]),
        pltpu.make_async_copy(down_hbm.at[0], w_out, w_sem.at[2]),
    ]
    for copy in weights:
        copy.start()
    for copy in smalls:
        copy.wait()

    values = tok_ref[...].astype(jnp.float32)
    centred = values - jnp.mean(values, axis=1, keepdims=True)
    variance = jnp.mean(centred * centred, axis=1, keepdims=True)
    normed = (centred * lax.rsqrt(variance + eps_norm) * gain_ref[...]).astype(jnp.bfloat16)
    for q in range(CHUNKS):
        xa[q, 0, 0] = normed[:, q * CHUNK:(q + 1) * CHUNK]

    def send(src, dst, send_sem, recv_sem, peer):
        pltpu.make_async_remote_copy(
            src_ref=src, dst_ref=dst, send_sem=send_sem, recv_sem=recv_sem,
            device_id=(peer,), device_id_type=MESH,
        ).start()

    def to_neighbours(q, d):
        for step in (1, 3):
            send(
                xa.at[q, 0, d], xa.at[q, 4 - step, d], sn.at[q, step, d], rn.at[q, 4 - step, d],
                line_peer((q + 1) % 3, step, c),
            )

    ids = ids_ref[...]
    scores = score_ref[...]
    exp_scores = jnp.exp(scores - jnp.max(scores, axis=0, keepdims=True))
    mixing = exp_scores / jnp.sum(exp_scores, axis=0, keepdims=True) * prob_ref[...]
    expert = iota((128, TOK), 0)
    matches = [ids[k:k + 1] == expert for k in range(4)]
    named = sum(jnp.where(match, 1.0, 0.0) for match in matches)
    earlier = jnp.where(iota((TOK, TOK), 0) < iota((TOK, TOK), 1), 1.0, 0.0)
    rank = jnp.dot(
        named.astype(jnp.bfloat16), earlier.astype(jnp.bfloat16),
        preferred_element_type=jnp.float32,
    )
    spread[...] = jnp.zeros((8, 128), jnp.float32)
    for k in range(4):
        slot = jnp.sum(jnp.where(matches[k], rank, 0.0), axis=0, keepdims=True)
        spread[k:k + 1, 0:TOK] = ids[k:k + 1].astype(jnp.float32) * 16.0 + slot
        spread[4 + k:5 + k, 0:TOK] = mixing[k:k + 1]
    own = spread[...]
    own = own + pltpu.roll(own, TOK, 1)
    own = own + pltpu.roll(own, 2 * TOK, 1)
    quarter = ((iota((8, 128), 1) >> 5) * 4).astype(jnp.float32)
    own = own + jnp.where(iota((8, 128), 0) < 4, quarter, 0.0)
    for q in range(CHUNKS):
        aux[q, 0] = own

    pl.semaphore_wait(barrier, 19)
    for step in (2, 1, 3):
        for q in range(CHUNKS):
            send(
                aux.at[q, 0], aux.at[q, 4 - step], sa.at[q, step], ra.at[q, 4 - step],
                line_peer(q, step, c),
            )
    for step in (2, 1, 3):
        for q in range(CHUNKS):
            send(
                xa.at[q, 0, 0], xa.at[q, 0, 4 - step], s1.at[q, step], r1.at[q, 4 - step],
                line_peer(q, step, c),
            )
    for q in range(CHUNKS):
        to_neighbours(q, 0)

    def whole(ref, send_sem, recv_sem):
        return pltpu.make_async_remote_copy(
            src_ref=ref, dst_ref=ref, send_sem=send_sem, recv_sem=recv_sem,
            device_id=(me,), device_id_type=MESH,
        )

    def bulk(ref, j, h, send_sem, recv_sem):
        return whole(ref.at[j, pl.ds(0, 15 + h)], send_sem.at[h, j], recv_sem.at[h, j])

    def row_code(q, h, shape, dim):
        r = iota(shape, dim)
        low = r & 15
        a, b = (plane[q][0] + (r >> 6)) & 3, (plane[q][1] + (r >> 4)) & 3
        core = c if h == 0 else other
        return (plane_peer(q, a, b, core) * 16 + low).astype(jnp.float32)

    def exchange(h, part):
        core = c if h == 0 else other
        last = h == 1 and part is PARTS[-1]

        def body(t, carry):
            for j in part:
                q = j % 3
                turn = t if last else (t * STRIDE[q]) % 16
                a, b = turn // 4, turn % 4
                send(
                    ob.at[j, h * 16 + turn],
                    gb.at[j, h * 16 + ((4 - a) % 4) * 4 + (4 - b) % 4],
                    s3.at[h, j], r3.at[h, j],
                    plane_peer(q, rel(plane[q][0], a), rel(plane[q][1], b), core),
                )
            return carry

        if last:
            for t in FAR:
                body(t, 0)
        else:
            lax.fori_loop(1 - h, 16, body, 0)
        if h == 0:
            for j in part:
                gb[j, 0] = ob[j, 0]

    for q in range(CHUNKS):
        for d in (1, 3, 2):
            whole(aux.at[q, d], sa.at[q, d], ra.at[q, d]).wait_recv()
    group = iota((8, 128), 1) >> 5
    for q in range(CHUNKS):
        found = aux[q, 0]
        for d in range(1, LINE):
            found = jnp.where(group == d, aux[q, d], found)
        codes[q, 0] = found
    for step in (2, 1, 3):
        for q in range(CHUNKS):
            send(
                codes.at[q, 0], codes.at[q, 4 - step], sl.at[q, step], rl.at[q, 4 - step],
                line_peer((q + 1) % 3, step, c),
            )
    for d in (1, 3, 2):
        for q in range(CHUNKS):
            whole(xa.at[q, 0, d], s1.at[q, d], r1.at[q, d]).wait_recv()
            to_neighbours(q, d)

    half = CHUNK // 2

    def select(e):
        for q in range(CHUNKS):
            r = iota((128, 128), 0)
            h, step = r >> 6, (r >> 4) & 3
            core = c + h - 2 * c * h
            want = (line_peer((q + 2) % 3, step, core) * 16 + (r & 15)).astype(jnp.float32)
            found = codes[q, e]
            hit = found[0:1] == want
            for k in range(1, 4):
                hit = hit | (found[k:k + 1] == want)
            rows = jnp.dot(
                one_hot(hit), xa[q, e].reshape(LINE * TOK, CHUNK),
                preferred_element_type=jnp.float32,
            )
            sb[q, e] = rows.astype(jnp.bfloat16).reshape(2, LINE, 16, CHUNK)

    def deliver(h, e):
        core = c if h == 0 else other
        for step in (2, 1, 3, 0):
            for q in range(CHUNKS):
                if h == 0 and step == 0:
                    rb[q, 0, 0, e] = sb[q, e, 0, 0]
                    continue
                for low in (0, half):
                    send(
                        sb.at[q, e, h, step, :, pl.ds(low, half)],
                        rb.at[q, h, (4 - step) % 4, e, :, pl.ds(low, half)],
                        s2.at[q, h], r2.at[q, h], line_peer((q + 2) % 3, step, core),
                    )

    for d in (0,):
        for q in range(CHUNKS):
            for step, low in ((3, 0), (1, half)):
                e = 4 - step
                whole(xa.at[q, e, d], sn.at[q, e, d], rn.at[q, e, d]).wait_recv()
                send(
                    xa.at[q, e, d, :, pl.ds(low, half)], xa.at[q, 2, d, :, pl.ds(low, half)],
                    sn.at[q, 2, 0], rn.at[q, 2, 0], line_peer((q + 1) % 3, step, c),
                )
    select(0)
    deliver(0, 0)
    for d in (1, 3, 2):
        for q in range(CHUNKS):
            for step, low in ((3, 0), (1, half)):
                e = 4 - step
                whole(xa.at[q, e, d], sn.at[q, e, d], rn.at[q, e, d]).wait_recv()
                send(
                    xa.at[q, e, d, :, pl.ds(low, half)], xa.at[q, 2, d, :, pl.ds(low, half)],
                    sn.at[q, 2, 0], rn.at[q, 2, 0], line_peer((q + 1) % 3, step, c),
                )
    for q in range(CHUNKS):
        for e in (1, 3, 2):
            whole(codes.at[q, e], sl.at[q, e], rl.at[q, e]).wait_recv()
    for e in (1, 3):
        select(e)
        deliver(0, e)
    for q in range(CHUNKS):
        whole(xa.at[q, 2], sn.at[q, 2, 0], rn.at[q, 2, 0]).wait_recv()
    select(2)
    deliver(0, 2)
    for e in (0, 1, 3, 2):
        deliver(1, e)

    for q in range(CHUNKS):
        cols = jnp.transpose(
            jnp.concatenate([codes[q, 0], jnp.zeros((120, 128), jnp.float32)], axis=0)
        )
        for h in range(2):
            want = row_code(q, h, (128, ROWS), 1)
            factor = jnp.zeros((128, ROWS), jnp.float32)
            for k in range(4):
                factor = jnp.where(cols[:, k:k + 1] == want, cols[:, 4 + k:5 + k], factor)
            high = factor.astype(jnp.bfloat16)
            wm[q, h, 0:128] = high
            wm[q, h, 128:256] = (factor - high.astype(jnp.float32)).astype(jnp.bfloat16)

    square = (ROWS, ROWS)

    def arrived(q, o):
        zz, yy, xx, slot = o >> 6, (o >> 4) & 3, (o >> 2) & 3, o & 3
        if q == 1:
            return xx * 64 + zz * 16 + yy * 4 + slot
        return yy * 64 + xx * 16 + zz * 4 + slot

    def leaving(q, o):
        zz, yy, xx, slot = o >> 6, (o >> 4) & 3, (o >> 2) & 3, o & 3
        if q == 1:
            return zz * 64 + xx * 16 + yy * 4 + slot
        return xx * 64 + yy * 16 + zz * 4 + slot

    gather_order = [None] + [
        one_hot(arrived(q, iota(square, 0)) == iota(square, 1)) for q in (1, 2)
    ]
    spread_order = [None] + [
        one_hot(leaving(q, iota(square, 1)) == iota(square, 0)) for q in (1, 2)
    ]

    def ordered(order, rows):
        if order is None:
            return rows
        return jnp.dot(order, rows, preferred_element_type=jnp.float32).astype(jnp.bfloat16)

    for copy in weights:
        copy.wait()
    for h in range(2):
        for q in range(CHUNKS):
            part = rb.at[q, h] if h else rb.at[q, 0, pl.ds(0, 3)]
            whole(part, s2.at[q, h], r2.at[q, h]).wait_recv()
        for q in range(CHUNKS):
            rows = rb[q, h].reshape(ROWS, CHUNK)
            xp[:, q * CHUNK:(q + 1) * CHUNK] = ordered(gather_order[q], rows)
        acts = jnp.dot(xp[...], w_in[...], preferred_element_type=jnp.float32)
        gate_act, up_act = acts[:, :FFE], acts[:, FFE:]
        hidden = (gate_act * jax.nn.sigmoid(gate_act) * up_act).astype(jnp.bfloat16)
        hidden = [ordered(spread_order[q], hidden) for q in range(CHUNKS)]
        for part in PARTS:
            for j in part:
                made = jnp.dot(
                    hidden[j % 3], w_out[:, columns(j)], preferred_element_type=jnp.float32
                )
                ob[j, h * 16:(h + 1) * 16] = made.astype(jnp.bfloat16).reshape(16, 16, PIECE)
            exchange(h, part)

    def here(j, slot):
        return parts_ref.at[slot, :, pl.ds(columns(j).start, PIECE)]

    def summed(j, h):
        rows = gb[j, h * 16:(h + 1) * 16].reshape(ROWS, PIECE)
        both = jnp.dot(wm[j % 3, h], rows, preferred_element_type=jnp.float32)
        return both[0:128] + both[128:256]

    for part in PARTS:
        for j in part:
            bulk(gb, j, 0, s3, r3).wait_recv()
        for j in part:
            tsum[j] = summed(j, 0)
    for part in PARTS:
        for j in part:
            bulk(gb, j, 1, s3, r3).wait_recv()
        for j in part:
            total = tsum[j] + summed(j, 1)
            tb[j] = total.astype(jnp.bfloat16).reshape(LINE, TOK, PIECE)
        for d in (2, 1, 3):
            for j in part:
                send(
                    tb.at[j, d], here(j, 4 - d), s4.at[j], r4.at[j], line_peer(j % 3, d, c)
                )
        for j in part:
            pltpu.make_async_copy(tb.at[j, 0], here(j, 0), own_sem.at[j]).start()

    for q in range(CHUNKS):
        for d in range(LINE):
            if d > 0:
                whole(aux.at[q, d], sa.at[q, d], ra.at[q, d]).wait_send()
                whole(codes.at[q, d], sl.at[q, d], rl.at[q, d]).wait_send()
                whole(xa.at[q, 0, d], s1.at[q, d], r1.at[q, d]).wait_send()
            for e in (1, 3):
                whole(xa.at[q, e, d], sn.at[q, e, d], rn.at[q, e, d]).wait_send()
        whole(xa.at[q, 2], sn.at[q, 2, 0], rn.at[q, 2, 0]).wait_send()
        for h in range(2):
            part = rb.at[q, h] if h else rb.at[q, 0, pl.ds(0, 3)]
            whole(part, s2.at[q, h], r2.at[q, h]).wait_send()
    for j in range(PIECES):
        for h in range(2):
            bulk(ob, j, h, s3, r3).wait_send()
        whole(tb.at[j, pl.ds(0, 3)], s4.at[j], r4.at[j]).wait()
        pltpu.make_async_copy(tb.at[j, 0], here(j, 0), own_sem.at[j]).wait()


def local(
    tokens, norm_gain, expert_ids, expert_scores, group_prob, gate_weight, up_weight, down_weight
):
    hbm = pl.BlockSpec(memory_space=pl.ANY)
    bf16, f32 = jnp.bfloat16, jnp.float32
    dma = pltpu.SemaphoreType.DMA
    width = CHUNKS * CHUNK
    rows = pltpu.VMEM((PIECES, 32, 16, PIECE), bf16)
    line = (CHUNKS, LINE)
    parts = pl.pallas_call(
        step_kernel,
        out_shape=jax.ShapeDtypeStruct((LINE, TOK, width), bf16),
        in_specs=[hbm] * 8,
        out_specs=hbm,
        scratch_shapes=[
            pltpu.VMEM((TOK, width), bf16),
            pltpu.VMEM((1, width), f32),
            pltpu.VMEM((4, TOK), jnp.int32),
            pltpu.VMEM((4, TOK), f32),
            pltpu.VMEM((1, TOK), f32),
            pltpu.VMEM((8, 128), f32),
            pltpu.VMEM((width, 2 * FFE), bf16),
            pltpu.VMEM((FFE, width), bf16),
            pltpu.VMEM(line + (LINE, TOK, CHUNK), bf16),
            pltpu.VMEM(line + (8, 128), f32),
            pltpu.VMEM(line + (8, 128), f32),
            pltpu.VMEM(line + (2, LINE, 16, CHUNK), bf16),
            pltpu.VMEM((CHUNKS, 2, LINE, LINE, 16, CHUNK), bf16),
            pltpu.VMEM((ROWS, width), bf16),
            rows,
            rows,
            pltpu.VMEM((PIECES, LINE * TOK, PIECE), f32),
            pltpu.VMEM((PIECES, LINE, TOK, PIECE), bf16),
            pltpu.VMEM((CHUNKS, 2, 256, ROWS), bf16),
            dma((5,)), dma((3,)), dma((PIECES,)),
            dma(line), dma(line),
            dma(line), dma(line),
            dma(line), dma(line),
            dma(line + (LINE,)), dma(line + (LINE,)),
            dma((CHUNKS, 2)), dma((CHUNKS, 2)),
            dma((2, PIECES)), dma((2, PIECES)),
            dma((PIECES,)), dma((PIECES,)),
        ],
        compiler_params=pltpu.CompilerParams(
            collective_id=0, has_side_effects=True, vmem_limit_bytes=60 * 2**20
        ),
        name="expert_step",
    )(
        tokens, norm_gain[None, :], expert_ids.T, expert_scores.T, group_prob[None, :],
        gate_weight, up_weight, down_weight,
    )
    terms = [parts[s].astype(f32) for s in range(LINE)]
    return ((terms[0] + terms[1]) + (terms[2] + terms[3])).astype(bf16)


def solution(mesh):
    in_specs = (
        P("ep", None),
        P(),
        P("ep", None),
        P("ep", None),
        P("ep"),
        P("ep", None, None),
        P("ep", None, None),
        P("ep", None, None),
    )
    out_specs = P("ep", None)
    return jax.shard_map(local, mesh=mesh, in_specs=in_specs, out_specs=out_specs, check_vma=False)
```
